32 devices in a mesh: grp: 2 (over x), ep: 8 (over z, y), tp: 2 (over core).
Axes of the slice: x: 2, y: 2, z: 4, core: 2. Of those that a mesh axis runs over, the one named last changes fastest.
Arguments:
- tokens: bfloat16 [1024, 2048], P(('grp', 'ep')), parts along dimension 0, may hold values from -6 to 6
- norm_gain: float32 [2048], replicated, may hold values from 0.1 to 1.9
- groups: int32 [1024], P(('grp', 'ep')), parts along dimension 0, may hold values from 0 to 1, as said below
- picks: int32 [1024, 4], P(('grp', 'ep')), parts along dimension 0, may hold values from 0 to 7, as said below
- gates: float32 [1024, 4], P(('grp', 'ep')), parts along dimension 0, may hold values from 0.1 to 1
- w_gate: bfloat16 [16, 2048, 512], P('ep', None, 'tp'), may hold values from -0.125 to 0.125
- w_up: bfloat16 [16, 2048, 512], P('ep', None, 'tp'), may hold values from -0.125 to 0.125
- w_down: bfloat16 [16, 512, 2048], P('ep', 'tp'), may hold values from -0.25 to 0.25
Outputs:
- mixed: bfloat16 [1024, 2048], P(('grp', 'ep'), 'tp'), parts along dimension 0
The draws below stay inside these ranges and needn't reach their ends.
There are 2 independent parts, one for each index of `grp`. The reference program is written for one: setup_inputs(seed, part) draws one part's arguments, and reference() takes and returns one part's arrays. A program takes and returns all parts, laid end to end along the dimension named above; an argument that names none is the same for every part. Nothing has to cross between parts.
Inputs may be any that keep to these rules, and one draw needn't show every extreme that they name: `groups`: among the tokens of one device, exactly 32 lie in one common group and all of them name one common expert of it as their first pick; every other token of that device lies in another group. A token's 4 picks are distinct. Among the tokens of one device at most 32 name any one expert (group and pick together), and in every draw one expert is named by exactly 32 tokens of every device.
All inputs are finite; a program needn't handle non-finite values.
Results may differ from the reference program's by a relative error of at most 0.014.
Values may be sent and summed in bfloat16 or wider, within the bound.
A program may use at most 64 MiB of HBM per device.

```python
import math
import jax
import jax.numpy as jnp
from jax import lax

D = 2048
FFE = 512
GROUPS = 2
TOP_K = 4
TOK_DEV = 64
EXPERTS = 16
GROUP_EXPERTS = 8
CAP = 32
TOKENS = 512
N_EP = 8
N_TP = 2


def routing_tables(key):
    base = jax.random.fold_in(key, 7)
    keys = jax.random.split(base, 3)
    hot_group = jax.random.randint(keys[0], (), 0, GROUPS)
    hot_expert = jax.random.randint(keys[1], (), 0, GROUP_EXPERTS)
    slot = jnp.arange(TOP_K, dtype=jnp.int32)

    def one_block(block_key):
        key_perm, key_hot, key_rest, key_group = jax.random.split(block_key, 4)
        order = jax.random.permutation(key_perm, TOK_DEV).astype(jnp.int32)
        offset_hot = jax.random.randint(key_hot, (), 0, GROUP_EXPERTS - 1)
        offset_rest = jax.random.randint(key_rest, (), 0, GROUP_EXPERTS)
        other = (hot_group + 1 + jax.random.randint(key_group, (TOK_DEV,), 0, GROUPS - 1)) % GROUPS
        is_hot = order < CAP
        step_hot = order[:, None] * (TOP_K - 1) + slot[None, :] - 1
        hot_values = jnp.where(slot[None, :] == 0, hot_expert, (hot_expert + 1 + (offset_hot + step_hot) % (GROUP_EXPERTS - 1)) % GROUP_EXPERTS)
        step_rest = (order[:, None] - CAP) * TOP_K + slot[None, :]
        rest_values = (offset_rest + step_rest) % GROUP_EXPERTS
        chosen = jnp.where(is_hot[:, None], hot_values, rest_values)
        group_of = jnp.where(is_hot, hot_group, other)
        return (group_of.astype(jnp.int32), chosen.astype(jnp.int32))
    block_keys = jax.random.split(keys[2], TOKENS // TOK_DEV)
    group_of, chosen = jax.vmap(one_block)(block_keys)
    return (group_of.reshape(TOKENS), chosen.reshape(TOKENS, TOP_K))


def draw_groups(key, part):
    return routing_tables(key)[0]


def draw_picks(key, part):
    return routing_tables(key)[1]


def block_scale(rng, shape, cuts, low, high):
    factor_of, own = 1.0, jax.random.fold_in(rng, 6)
    for dim, blocks in cuts:
        steps = jnp.exp(jax.random.uniform(jax.random.fold_in(own, dim), (blocks,), jnp.float32, low / len(cuts), high / len(cuts)))
        factor_of = factor_of * jnp.repeat(steps, shape[dim] // blocks).reshape([-1 if axis == dim else 1 for axis in range(len(shape))])
    return factor_of


def bell_draw(own_key, dims, scale, bound, shards=(), kind=jnp.bfloat16):
    result = scale * jax.random.normal(own_key, dims, jnp.float32)
    if shards:
        result = result * block_scale(own_key, dims, shards, -0.22, 0.18)
    return jnp.clip(result, -bound, bound).astype(kind)


def setup_inputs(seed: int = 0, part: int = 0) -> dict:
    key_list = jax.random.split(jax.random.key(seed), 9)
    own_keys = jax.random.split(jax.random.fold_in(key_list[8], part), 9)
    tokens = bell_draw(own_keys[0], (TOKENS, D), 1.0, 6.0, ((0, 8),))
    norm_gain = jnp.clip(1.0 + 0.18 * jax.random.normal(key_list[1], (D,), jnp.float32), 0.1, 1.9)
    groups = draw_groups(jax.random.fold_in(jax.random.fold_in(key_list[8], part), 71), part)
    picks = draw_picks(jax.random.fold_in(jax.random.fold_in(key_list[8], part), 71), part)
    gates = jnp.clip(jnp.exp(math.log(1.0) - 2.3025851 * jax.random.uniform(own_keys[4], (TOKENS, TOP_K), jnp.float32) ** block_scale(own_keys[4], (TOKENS, TOP_K), ((0, 8),), -0.2, 0.2)), 0.1, 1.0)
    w_gate = bell_draw(key_list[5], (EXPERTS, D, FFE), D ** -0.5, 0.125, ((0, 8), (2, 2)))
    w_up = bell_draw(key_list[6], (EXPERTS, D, FFE), D ** -0.5, 0.125, ((0, 8), (2, 2)))
    w_down = bell_draw(key_list[7], (EXPERTS, FFE, D), FFE ** -0.5, 0.25, ((0, 8), (1, 2)))
    return dict(tokens=tokens, norm_gain=norm_gain, groups=groups, picks=picks, gates=gates, w_gate=w_gate, w_up=w_up, w_down=w_down)


epsilon = 1e-06

def reference(tokens, norm_gain, groups, picks, gates, w_gate, w_up, w_down):
    values = tokens.astype(jnp.float32)
    normed = (values * lax.rsqrt(lax.optimization_barrier(jnp.mean(values * values, axis=-1, keepdims=True)) + epsilon) * norm_gain.astype(jnp.float32)).astype(jnp.bfloat16)
    expert_id = groups[:, None] * GROUP_EXPERTS + picks
    limit = N_EP * CAP
    slots = jnp.arange(limit, dtype=jnp.int32)

    def per_expert(total, inputs):
        expert, wg, wu, wd = inputs
        hit = expert_id == expert
        gate_me = lax.optimization_barrier(jnp.sum(jnp.where(hit, gates, 0.0), axis=1))
        present = jnp.any(hit, axis=1)
        position = jnp.cumsum(present.astype(jnp.int32)) - 1
        select = jnp.logical_and(position[None, :] == slots[:, None], present[None, :]).astype(jnp.float32)
        rows = jnp.dot(select.astype(jnp.bfloat16), normed, preferred_element_type=jnp.float32).astype(jnp.bfloat16)
        gate_pre = jnp.dot(rows, wg, preferred_element_type=jnp.float32)
        up_pre = jnp.dot(rows, wu, preferred_element_type=jnp.float32)
        hidden = (jax.nn.silu(gate_pre) * up_pre).astype(jnp.bfloat16)
        blocks = hidden.reshape(limit, N_TP, FFE // N_TP).astype(jnp.float32)
        down = wd.reshape(N_TP, FFE // N_TP, D).astype(jnp.float32)
        parts = jnp.einsum('rkf,kfd->krd', blocks, down).astype(jnp.bfloat16)
        expert_out = lax.optimization_barrier(jnp.sum(parts.astype(jnp.float32), axis=0)).astype(jnp.bfloat16)
        weighted = (select * gate_me[None, :]).T
        return (total + jnp.dot(weighted, expert_out.astype(jnp.float32), precision=lax.Precision.HIGHEST), None)
    start = jnp.zeros((tokens.shape[0], D), jnp.float32)
    total, unused = lax.scan(per_expert, start, (jnp.arange(EXPERTS, dtype=jnp.int32), w_gate, w_up, w_down))
    return total.astype(jnp.bfloat16)
```

```python
import functools
import math

import jax
import jax.numpy as jnp
from jax import lax
from jax.experimental import pallas as pl
from jax.experimental.pallas import tpu as pltpu
from jax.sharding import PartitionSpec as P

GROUPS = 2
MESH = pl.DeviceIdType.MESH
EPS = 1e-06
EXT = 128
PIECES = 2
F32 = jnp.float32
BF16 = jnp.bfloat16


def kernel(
    dims,
    tok_hbm,
    gain_hbm,
    grp_hbm,
    pick_hbm,
    gate_hbm,
    wg_hbm,
    wu_hbm,
    wd_hbm,
    out_ref,
    tok_ref,
    gain_ref,
    grp_ref,
    pick_ref,
    gate_ref,
    wg,
    wu,
    wd,
    xbuf,
    cross_out,
    psend,
    precv,
    ymine,
    rsend,
    rrecv,
    csend,
    crecv,
    w_sem,
    x_send,
    x_recv,
    d_send,
    d_recv,
    p_send,
    p_recv,
    r_send,
    r_recv,
    c_send,
    c_recv,
):
    members, gcap, local, top, width, chunk = dims
    tokens = tok_ref.shape[0]
    half = gcap // 2
    cols = width // 2
    pcols = cols // PIECES
    full = width + EXT
    cuts = [width // PIECES * p for p in range(PIECES)] + [full]
    ep = lax.axis_index("ep")
    c = lax.axis_index("tp")
    g = ep // members
    m = ep % members
    cross_ep = (1 - g) * members + m
    rows_c = pl.ds(pl.multiple_of(c * half, half), half)

    def member(i):
        return {"ep": g * members + i, "tp": c}

    mate = {"ep": ep, "tp": 1 - c}
    cross = {"ep": cross_ep, "tp": c}

    barrier = pltpu.get_barrier_semaphore()
    peers = [member((m + d) % members) for d in range(1, members)] + [mate, cross]
    for peer in peers:
        pl.semaphore_signal(barrier, inc=1, device_id=peer, device_id_type=MESH)
    pairs = (
        (grp_hbm, grp_ref),
        (pick_hbm, pick_ref),
        (gate_hbm, gate_ref),
        (gain_hbm, gain_ref),
        (tok_hbm, tok_ref),
        (wg_hbm, wg),
        (wu_hbm, wu),
        (wd_hbm, wd),
    )
    loads = [
        pltpu.make_async_copy(src, dst, w_sem.at[i]) for i, (src, dst) in enumerate(pairs)
    ]
    for load in loads:
        load.start()
    for load in loads[:3]:
        load.wait()

    mine_row = jnp.broadcast_to(grp_ref[...] == g, (8, tokens)).astype(F32)
    tri = (
        lax.broadcasted_iota(jnp.int32, (tokens, tokens), 0)
        < lax.broadcasted_iota(jnp.int32, (tokens, tokens), 1)
    ).astype(F32)
    rank = jnp.dot(mine_row, tri, preferred_element_type=F32)[0:1, :]
    mine = mine_row[0:1, :]
    col = lax.broadcasted_iota(jnp.int32, (1, tokens), 1).astype(F32)
    slot_row = lax.broadcasted_iota(jnp.int32, (gcap, tokens), 0).astype(F32)
    sel_own = jnp.where(slot_row == rank, mine, 0.0)
    sel_oth = jnp.where(slot_row == col - rank, 1.0 - mine, 0.0)
    half_row = (lax.broadcasted_iota(jnp.int32, (half, tokens), 0) + c * half).astype(F32)
    sel_oth_half = jnp.where(half_row == col - rank, 1.0 - mine, 0.0)

    line = lax.broadcasted_iota(jnp.int32, (EXT, tokens), 0)
    spread = jnp.zeros((EXT, tokens), F32)
    for j in range(top):
        spread += jnp.where(pick_ref[j : j + 1, :] == line % (EXT // 2), gate_ref[j : j + 1, :], 0.0)
    high = spread.astype(BF16).astype(F32)
    ext = jnp.where(line < EXT // 2, high, spread - high).astype(BF16)
    pick_half = sel_oth_half.astype(BF16)
    pick_own = sel_own.astype(BF16)
    last = (((1,), (1,)), ((), ()))
    cross_out[:, width:] = lax.dot_general(
        pick_half, ext, last, preferred_element_type=F32
    ).astype(BF16)
    for load in loads[3:5]:
        load.wait()
    values = tok_ref[...].astype(F32)
    scale = lax.rsqrt(jnp.mean(values * values, axis=-1, keepdims=True) + EPS)
    normed = (values * scale * gain_ref[...]).astype(BF16)
    cross_out[:, :width] = jnp.dot(pick_half, normed, preferred_element_type=F32).astype(BF16)

    pl.semaphore_wait(barrier, len(peers))
    def span(p):
        return pl.ds(cuts[p], cuts[p + 1] - cuts[p])

    sends = []
    for p in range(PIECES):
        copy = pltpu.make_async_remote_copy(
            src_ref=cross_out.at[:, span(p)],
            dst_ref=xbuf.at[members + m, rows_c, span(p)],
            send_sem=c_send.at[0, p],
            recv_sem=x_recv.at[members + m, p],
            device_id=cross,
            device_id_type=MESH,
        )
        copy.start()
        sends.append(copy)

    xbuf[m, :, width:] = lax.dot_general(
        pick_own, ext, last, preferred_element_type=F32
    ).astype(BF16)
    xbuf[m, :, :width] = jnp.dot(pick_own, normed, preferred_element_type=F32).astype(BF16)

    def x_copy(slot, p, dest, sem):
        return pltpu.make_async_remote_copy(
            src_ref=xbuf.at[slot, rows_c, span(p)],
            dst_ref=xbuf.at[slot, rows_c, span(p)],
            send_sem=x_send.at[sem, p],
            recv_sem=x_recv.at[slot, p],
            device_id=dest,
            device_id_type=MESH,
        )

    def d_copy(slot, p, which):
        rows = pl.ds(pl.multiple_of(which * half, half), half)
        return pltpu.make_async_remote_copy(
            src_ref=xbuf.at[slot, rows, span(p)],
            dst_ref=xbuf.at[slot, rows, span(p)],
            send_sem=d_send.at[slot, p],
            recv_sem=d_recv.at[slot, p],
            device_id=mate,
            device_id_type=MESH,
        )

    def start(copy):
        copy.start()
        sends.append(copy)

    for p in range(PIECES):
        for d in range(1, members):
            start(x_copy(m, p, member((m + d) % members), d))
    for p in range(PIECES):
        for d in range(1, members):
            slot = (m + members - d) % members
            x_copy(slot, p, mate, 0).wait_recv()
            start(d_copy(slot, p, c))
    for p in range(PIECES):
        x_copy(members + m, p, mate, 0).wait_recv()
        for d in range(1, members):
            start(x_copy(members + m, p, member((m + d) % members), members + d))
        start(d_copy(members + m, p, c))
    for p in range(PIECES):
        for d in range(1, members):
            d_copy((m + members - d) % members, p, 1 - c).wait_recv()
    for load in loads[5:]:
        load.wait()

    per = chunk // gcap
    lane_x = lax.broadcasted_iota(jnp.int32, (chunk, EXT), 1)
    steps = members * gcap // chunk
    kcut = width // PIECES

    def chunk_rows(i):
        return pl.ds(i * chunk, chunk)

    def wide(core, p):
        return pl.ds(pl.multiple_of(core * cols + p * pcols, pcols), pcols)

    def compute(part, ready):
        def body(i, wait):
            blocks = pl.ds(part * members + i * per, per)
            gate_pre = [jnp.zeros((chunk, wg.shape[2]), F32) for _ in range(local)]
            up_pre = [jnp.zeros((chunk, wg.shape[2]), F32) for _ in range(local)]
            for p in range(PIECES):
                wait(p)
                k = pl.ds(p * kcut, kcut)
                rows = xbuf[blocks, :, k].reshape(chunk, kcut)
                for j in range(local):
                    gate_pre[j] += jnp.dot(rows, wg[j, k], preferred_element_type=F32)
                    up_pre[j] += jnp.dot(rows, wu[j, k], preferred_element_type=F32)
            tail = xbuf[blocks, :, width:].reshape(chunk, EXT).astype(F32)
            hidden = []
            for j in range(local):
                weight = jnp.sum(
                    jnp.where(lane_x % (EXT // 2) == m * local + j, tail, 0.0),
                    axis=1,
                    keepdims=True,
                )
                act = gate_pre[j] / (1.0 + jnp.exp(-gate_pre[j])) * up_pre[j]
                hidden.append((act * weight).astype(BF16))

            def down(core, p):
                total = jnp.zeros((chunk, pcols), F32)
                for j in range(local):
                    total += jnp.dot(hidden[j], wd[j, :, wide(core, p)], preferred_element_type=F32)
                return total

            for p in range(PIECES):
                psend[part, p, chunk_rows(i)] = down(1 - c, p).astype(BF16)
                p_copy(part, p, i).start()
            for p in range(PIECES):
                ymine[part, p, chunk_rows(i)] = down(c, p)

        if steps == 1:
            body(0, ready)
        else:
            for p in range(PIECES):
                ready(p)

            def loop(i, carry):
                body(i, lambda p: None)
                return carry

            lax.fori_loop(0, steps, loop, 0)

    def p_copy(part, p, i):
        return pltpu.make_async_remote_copy(
            src_ref=psend.at[part, p, chunk_rows(i)],
            dst_ref=precv.at[part, p, chunk_rows(i)],
            send_sem=p_send.at[part, p, i],
            recv_sem=p_recv.at[part, p, i],
            device_id=mate,
            device_id_type=MESH,
        )

    def r_copy(part, p, to_slot, from_slot, dest, sem):
        return pltpu.make_async_remote_copy(
            src_ref=rsend.at[part, p, to_slot],
            dst_ref=rrecv.at[part, p, from_slot],
            send_sem=r_send.at[part, p, sem],
            recv_sem=r_recv.at[part, p, from_slot],
            device_id=dest,
            device_id_type=MESH,
        )

    def reduce_tp(part):
        for p in range(PIECES):

            def body(i, carry):
                p_copy(part, p, i).wait()
                total = ymine[part, p, chunk_rows(i)] + precv[part, p, chunk_rows(i)].astype(F32)
                rsend[part, p, pl.ds(i * per, per)] = total.astype(BF16).reshape(per, gcap, pcols)
                return carry

            if steps == 1:
                body(0, 0)
            else:
                lax.fori_loop(0, steps, body, 0)
            for d in range(1, members):
                dest = (m + d) % members
                start(r_copy(part, p, dest, m, member(dest), d))

    def collect(part, p):
        total = rsend[part, p, m].astype(F32)
        for d in range(1, members):
            slot = (m + members - d) % members
            r_copy(part, p, slot, slot, mate, 0).wait_recv()
            total += rrecv[part, p, slot].astype(F32)
        return total.astype(BF16)

    def relayed(p):
        for d in range(1, members):
            slot = members + (m + members - d) % members
            x_copy(slot, p, mate, 0).wait_recv()
            start(d_copy(slot, p, c))

    def crossed(p):
        for d in range(members):
            d_copy(members + (m + members - d) % members, p, 1 - c).wait_recv()

    compute(0, lambda p: None)
    for p in range(PIECES):
        relayed(p)
    reduce_tp(0)
    compute(1, crossed)
    reduce_tp(1)
    own = [collect(0, p) for p in range(PIECES)]
    back = []
    for p in range(PIECES):
        csend[p] = collect(1, p)
        copy = pltpu.make_async_remote_copy(
            src_ref=csend.at[p],
            dst_ref=crecv.at[p],
            send_sem=c_send.at[1, p],
            recv_sem=c_recv.at[p],
            device_id=cross,
            device_id_type=MESH,
        )
        copy.start()
        back.append(copy)
    turn = (((0,), (0,)), ((), ()))
    pick_oth = sel_oth.astype(BF16)
    mixed = [lax.dot_general(pick_own, own[p], turn, preferred_element_type=F32) for p in range(PIECES)]
    for copy in sends:
        copy.wait_send()
    for p in range(PIECES):
        back[p].wait()
        total = mixed[p] + lax.dot_general(pick_oth, crecv[p], turn, preferred_element_type=F32)
        out_ref[:, p * pcols : (p + 1) * pcols] = total.astype(BF16)


def on_device(tokens, norm_gain, groups, picks, gates, w_gate, w_up, w_down):
    tok_rows, width = tokens.shape
    top = picks.shape[1]
    local, _, ff = w_gate.shape
    senders = lax.axis_size("ep")
    members = senders // GROUPS
    hot = tok_rows * top // (senders * local // GROUPS)
    gcap = -(-max(hot, tok_rows - hot) // 32) * 32
    assert members * local <= EXT // 2
    chunk = max(gcap, min(128, members * gcap))
    steps = members * gcap // chunk
    pcols = width // 2 // PIECES
    full = width + EXT
    dims = (members, gcap, local, top, width, chunk)
    vmem = pl.BlockSpec(memory_space=pltpu.VMEM)
    hbm = pl.BlockSpec(memory_space=pl.ANY)
    dma = pltpu.SemaphoreType.DMA
    buffers = [
        ((tok_rows, width), BF16),
        ((1, width), F32),
        ((1, tok_rows), jnp.int32),
        ((top, tok_rows), jnp.int32),
        ((top, tok_rows), F32),
        ((local, width, ff), BF16),
        ((local, width, ff), BF16),
        ((local, ff, width), BF16),
        ((2 * members, gcap, full), BF16),
        ((gcap // 2, full), BF16),
        ((2, PIECES, members * gcap, pcols), BF16),
        ((2, PIECES, members * gcap, pcols), BF16),
        ((2, PIECES, members * gcap, pcols), F32),
        ((2, PIECES, members, gcap, pcols), BF16),
        ((2, PIECES, members, gcap, pcols), BF16),
        ((PIECES, gcap, pcols), BF16),
        ((PIECES, gcap, pcols), BF16),
    ]
    size = sum(math.prod(shape) * jnp.dtype(kind).itemsize for shape, kind in buffers)
    return pl.pallas_call(
        functools.partial(kernel, dims),
        out_shape=jax.ShapeDtypeStruct((tok_rows, width // 2), BF16),
        in_specs=[hbm] * 8,
        out_specs=vmem,
        scratch_shapes=[pltpu.VMEM(shape, kind) for shape, kind in buffers]
        + [
            dma((8,)),
            dma((2 * members, PIECES)),
            dma((2 * members, PIECES)),
            dma((2 * members, PIECES)),
            dma((2 * members, PIECES)),
            dma((2, PIECES, steps)),
            dma((2, PIECES, steps)),
            dma((2, PIECES, members)),
            dma((2, PIECES, members)),
            dma((2, PIECES)),
            dma((PIECES,)),
        ],
        compiler_params=pltpu.CompilerParams(
            collective_id=0, has_side_effects=True, vmem_limit_bytes=size + 8 * 2**20
        ),
    )(
        *(
            pltpu.with_memory_space_constraint(x, pltpu.HBM)
            for x in (
                tokens,
                norm_gain.reshape(1, width),
                groups.reshape(1, tok_rows),
                picks.T,
                gates.T,
                w_gate,
                w_up,
                w_down,
            )
        )
    )


def solution(mesh):
    in_specs = (
        P(("grp", "ep"), None),
        P(),
        P(("grp", "ep")),
        P(("grp", "ep"), None),
        P(("grp", "ep"), None),
        P("ep", None, "tp"),
        P("ep", None, "tp"),
        P("ep", "tp", None),
    )
    out_specs = P(("grp", "ep"), "tp")
    return jax.shard_map(
        on_device, mesh=mesh, in_specs=in_specs, out_specs=out_specs, check_vma=False
    )
```
